32 devices in a mesh: sp: 8 (over z, x), tp: 4 (over y, core).
Axes of the slice: x: 2, y: 2, z: 4, core: 2. Of those that a mesh axis runs over, the one named last changes fastest.
Arguments:
- residual: bfloat16 [2048, 2048], P('sp', 'tp'), may hold values from -26 to 26
- queries: bfloat16 [2048, 2048], P('tp', 'sp'), may hold values from -6 to 6
- keys: bfloat16 [2048, 2048], P('tp', 'sp'), may hold values from -6 to 6
- values: bfloat16 [2048, 2048], P('tp', 'sp'), may hold values from -12 to 12
- forget_cache: float32 [32, 2048], P('tp', 'sp'), as said below
- out_weight: bfloat16 [2048, 2048], P('tp'), may hold values from -0.125 to 0.125
- norm_gain: float32 [2048], replicated, may hold values from 0.1 to 1.9
- routes: int32 [2048, 2], P('sp'), may hold values from 0 to 7, all different within a row; in each aligned block of 256 rows (0 to 255, 256 to 511, ...) at most 80 rows name the same one
- route_weight: float32 [2048, 2], P('sp'), may hold values from 0.2 to 1
- gate_weight: bfloat16 [8, 2048, 4096], P('sp', None, 'tp'), may hold values from -0.125 to 0.125
- up_weight: bfloat16 [8, 2048, 4096], P('sp', None, 'tp'), may hold values from -0.125 to 0.125
- down_weight: bfloat16 [8, 4096, 2048], P('sp', 'tp'), may hold values from -0.09375 to 0.09375
Outputs:
- updated: bfloat16 [2048, 2048], P('sp', 'tp')
The draws below stay inside these ranges and needn't reach their ends.
Inputs may be any that keep to these rules, and one draw needn't show every extreme that they name: `routes`: each row names 2 different experts; within the 256 rows of one index of sp no expert is named by more than 80 rows, and in the rows of some index some expert is named by exactly 80. `forget_cache`: each head's row never rises from one position to the next.
All inputs are finite; a program needn't handle non-finite values.
Results may differ from the reference program's by a relative error of at most 0.013.
Values may be sent and summed in bfloat16 or wider, within the bound.
A program may use at most 64 MiB of HBM per device.

```python
import math
import jax
import jax.numpy as jnp
import numpy as np
from jax import lax

D = 2048
HEAD_TOTAL = 32
HEAD_DIM = 64
FF = 4096
TOPK = 2
TOK_DEV = 256
TOKEN_TOTAL = 2048
EXPERTS = 8
CAP = 80
GROUP_HEADS = 8
FF_PART = 1024
N_SP = 8
N_TP = 4


def draw_queries(key, part):
    full_shape = (HEAD_TOTAL * HEAD_DIM, TOKEN_TOTAL)
    drawn = jnp.clip(1.6 * jax.random.normal(jax.random.fold_in(key, 1), full_shape, jnp.float32), -6.0, 6.0)
    return drawn.astype(jnp.bfloat16)


def draw_keys(key, part):
    full_shape = (HEAD_TOTAL * HEAD_DIM, TOKEN_TOTAL)
    drawn = jnp.clip(1.6 * jax.random.normal(jax.random.fold_in(key, 2), full_shape, jnp.float32), -6.0, 6.0)
    return drawn.astype(jnp.bfloat16)


def draw_residual(key, part):
    sequence_lanes = jax.random.split(jax.random.fold_in(key, 3), 3)
    feature = jnp.arange(D, dtype=jnp.float32) / D - 0.5
    jitter = jnp.exp(jax.random.uniform(sequence_lanes[1], (D,), jnp.float32, jnp.log(0.7), jnp.log(1.4)))
    rising = jnp.exp(jnp.log(4.0) * feature) * jitter
    token_scale = jnp.exp(jax.random.uniform(sequence_lanes[2], (TOKEN_TOTAL, 1), jnp.float32, jnp.log(0.3), jnp.log(3.0)))
    drawn = jnp.clip(jax.random.normal(sequence_lanes[0], (TOKEN_TOTAL, D), jnp.float32), -3.0, 3.0)
    return (drawn * rising[None, :] * token_scale).astype(jnp.bfloat16)


def draw_forget_cache(key, part):
    sequence_lanes = jax.random.split(jax.random.fold_in(key, 4), 7)
    head_order = jax.random.permutation(sequence_lanes[0], HEAD_TOTAL)
    slow_count = HEAD_TOTAL // 2
    slow_total = jax.random.uniform(sequence_lanes[1], (HEAD_TOTAL,), jnp.float32, 0.3, 0.9)
    lagging_heads = head_order < slow_count
    fast_length = jax.random.uniform(sequence_lanes[2], (HEAD_TOTAL,), jnp.float32, 30.0, 100.0)
    base_rate = jnp.where(lagging_heads, slow_total / TOKEN_TOTAL, 1.0 / fast_length)
    block_factor = jnp.exp(jax.random.uniform(sequence_lanes[3], (HEAD_TOTAL, TOKEN_TOTAL // TOK_DEV), jnp.float32, jnp.log(0.5), jnp.log(2.0)))
    roughness = jnp.exp(jax.random.uniform(sequence_lanes[4], (HEAD_TOTAL, TOKEN_TOTAL), jnp.float32, jnp.log(0.5), jnp.log(2.0)))
    decay_speed = base_rate[:, None] * jnp.repeat(block_factor, TOK_DEV, axis=1) * roughness
    spike_locations = jax.random.randint(sequence_lanes[5], (2,), 0, TOKEN_TOTAL)
    spike_struck = jnp.any(jnp.arange(TOKEN_TOTAL, dtype=jnp.int32)[:, None] == spike_locations[None, :], axis=1)
    spike_retained = jnp.log(jax.random.uniform(sequence_lanes[6], (HEAD_TOTAL,), jnp.float32, 0.55, 0.8))
    gate_logarithm = -decay_speed + jnp.where(lagging_heads[:, None] & spike_struck[None, :], spike_retained[:, None], 0.0)
    return jnp.cumsum(gate_logarithm, axis=1).astype(jnp.float32)


def block_scale(rng, shape, cuts, low, high):
    def one(dim, shards_of):
        draws = jax.random.uniform(jax.random.fold_in(jax.random.fold_in(rng, 6), dim), (shards_of,), jnp.float32, low / len(cuts), high / len(cuts))
        return jnp.repeat(jnp.exp(draws), shape[dim] // shards_of).reshape((-1,) + (1,) * (len(shape) - dim - 1))

    level = one(*cuts[0])
    for cut in cuts[1:]:
        level = level * one(*cut)
    return level


def routed_block(stream_key, own, number, rows, count, top, limit, skew):
    order = jax.random.permutation(stream_key, count)
    packed, ordinary = shares(count, rows * top, limit, skew, True), shares(count, rows * top, limit, skew, False)
    places = jnp.arange(count)

    def named(sizes, rotation):
        used = int((sizes > 0).sum())
        fixed = max(1, used // 4)
        shifted = fixed + (places - fixed + rotation * (used - fixed)) % max(1, count - fixed)
        return jnp.zeros((count,), jnp.int32).at[order[jnp.where(places < fixed, places, shifted)]].set(jnp.asarray(sizes, jnp.int32))

    sizes = jnp.where(number % 4 == 0, named(packed, number // 4), named(ordinary, number - number // 4 - 1))
    mixed = jax.random.permutation(jax.random.fold_in(own, 3), count)
    giver, taker = mixed[0:count // 2 * 2:2], mixed[1:count // 2 * 2:2]
    room = jnp.minimum(sizes[giver] - 1, limit - sizes[taker]) // 2
    room = jnp.where((giver == order[0]) | (taker == order[0]) | (sizes[taker] == 0), 0, jnp.maximum(room, 0))
    shifted = jax.random.randint(jax.random.fold_in(own, 4), (count // 2,), 0, 1 << 20) % (room + 1)
    sizes = sizes.at[giver].add(-shifted).at[taker].add(shifted)
    labels = jnp.searchsorted(jnp.cumsum(sizes), jnp.arange(rows * top), side="right").astype(jnp.int32)
    listing = labels.reshape(top, rows).T
    listing = listing[jax.random.permutation(jax.random.fold_in(own, 1), rows)]
    rotation = jax.random.randint(jax.random.fold_in(own, 2), (rows, 1), 0, top)
    return jnp.take_along_axis(listing, (jnp.arange(top)[None, :] + rotation) % top, axis=1)


def shares(amount, total, reach, skew, full):
    weights = [(1 << 20) // math.isqrt(rank ** skew) + 1 for rank in range(1, amount + 1)]
    largest = reach if full else min(reach, max(-(-total // amount), total * weights[0] // sum(weights)))
    least = 1 if total - largest >= amount - 1 else 0
    counts, spare = [largest] + [least] * (amount - 1), total - largest - least * (amount - 1)
    while spare > 0:
        candidates = [i for i in range(1, amount) if counts[i] < largest] or [i for i in range(1, amount) if counts[i] < reach]
        whole, left = sum([weights[i] for i in candidates]), spare
        for i in candidates:
            more = min(reach - counts[i], max(1, left * weights[i] // whole), spare)
            counts[i] = counts[i] + more
            spare = spare - more
    return np.array(counts)


def bell_draw(stream_key, shape, scale, bound, pieces=(), kind=jnp.bfloat16):
    array = jax.random.normal(stream_key, shape, jnp.float32) * scale
    if len(pieces) > 0:
        array = block_scale(stream_key, shape, pieces, -0.22, 0.18) * array
    return jnp.clip(array, min=-bound, max=bound).astype(kind)


def setup_inputs(seed: int = 0) -> dict:
    seeds = jax.random.split(jax.random.key(seed), 13)
    residual = draw_residual(jax.random.fold_in(seeds[12], 71), 0)
    queries = draw_queries(jax.random.fold_in(seeds[12], 71), 0)
    keys = draw_keys(jax.random.fold_in(seeds[12], 71), 0)
    values = bell_draw(seeds[3], (HEAD_TOTAL * HEAD_DIM, TOKEN_TOTAL), 2.0, 12.0, ((0, 4), (1, 8)))
    forget_cache = draw_forget_cache(jax.random.fold_in(seeds[12], 71), 0)
    out_weight = bell_draw(seeds[5], (HEAD_TOTAL * HEAD_DIM, D), (HEAD_TOTAL * HEAD_DIM) ** -0.5, 0.125, ((0, 4),))
    norm_gain = jnp.clip(1.0 + 0.18 * jax.random.normal(seeds[6], (D,), jnp.float32), 0.1, 1.9)
    routes_keys = jax.random.split(jax.random.fold_in(seeds[7], 1), TOKEN_TOTAL // TOK_DEV)
    routes_turns = jax.random.permutation(jax.random.fold_in(seeds[7], 3), TOKEN_TOTAL // TOK_DEV)
    routes = jax.vmap(lambda own, number: routed_block(jax.random.fold_in(seeds[7], 2), own, number, TOK_DEV, EXPERTS, TOPK, CAP, 0))(routes_keys, routes_turns).reshape((TOKEN_TOTAL, TOPK))
    route_weight = jnp.clip(0.2 + 0.8 * jax.random.uniform(seeds[8], (TOKEN_TOTAL, TOPK), jnp.float32) ** block_scale(seeds[8], (TOKEN_TOTAL, TOPK), ((0, 8),), -0.2, 0.2), 0.2, 1.0)
    gate_weight = bell_draw(seeds[9], (EXPERTS, D, FF), D ** -0.5, 0.125, ((0, 8), (2, 4)))
    up_weight = bell_draw(seeds[10], (EXPERTS, D, FF), D ** -0.5, 0.125, ((0, 8), (2, 4)))
    down_weight = bell_draw(seeds[11], (EXPERTS, FF, D), FF ** -0.5, 0.09375, ((0, 8), (1, 4)))
    return {"residual": residual, "queries": queries, "keys": keys, "values": values, "forget_cache": forget_cache, "out_weight": out_weight, "norm_gain": norm_gain, "routes": routes, "route_weight": route_weight, "gate_weight": gate_weight, "up_weight": up_weight, "down_weight": down_weight}


norm_eps = 1e-06

def attend_head(operands):
    query_rows, key_rows, value_rows, cumulative = operands
    block_span = TOKEN_TOTAL // 8
    position = jnp.arange(TOKEN_TOTAL, dtype=jnp.int32)
    blocks = []
    for block_index in range(8):
        first_row = block_index * block_span
        end_row = first_row + block_span
        scores = jnp.dot(query_rows[:, first_row:end_row].T, key_rows[:, :end_row], preferred_element_type=jnp.float32) * HEAD_DIM ** (-0.5)
        scores = scores + cumulative[first_row:end_row, None] - cumulative[None, :end_row]
        allowed = position[None, :end_row] <= position[first_row:end_row, None]
        scores = jnp.where(allowed, scores, -jnp.inf)
        weights = jnp.exp(scores - lax.optimization_barrier(jnp.max(scores, axis=1, keepdims=True)))
        totals = lax.optimization_barrier(jnp.sum(weights, axis=1, keepdims=True))
        blocks.append(jnp.dot(weights.astype(jnp.bfloat16), value_rows[:, :end_row].T, preferred_element_type=jnp.float32) / totals)
    return jnp.concatenate(blocks, axis=0).astype(jnp.bfloat16)

def reference(residual, queries, keys, values, forget_cache, out_weight, norm_gain, routes, route_weight, gate_weight, up_weight, down_weight):
    query_heads = queries.reshape(HEAD_TOTAL, HEAD_DIM, TOKEN_TOTAL)
    key_heads = keys.reshape(HEAD_TOTAL, HEAD_DIM, TOKEN_TOTAL)
    value_heads = values.reshape(HEAD_TOTAL, HEAD_DIM, TOKEN_TOTAL)
    attended = lax.map(attend_head, (query_heads, key_heads, value_heads, forget_cache))
    attended = attended.transpose(1, 0, 2).reshape(TOKEN_TOTAL, HEAD_TOTAL * HEAD_DIM)
    group_width = GROUP_HEADS * HEAD_DIM

    def add_group(running, group_index):
        offset = (group_index * group_width).astype(jnp.int32)
        group_rows = lax.dynamic_slice_in_dim(attended, offset, group_width, 1)
        weight_rows = lax.dynamic_slice_in_dim(out_weight, offset, group_width, 0)
        group_part = lax.optimization_barrier(jnp.dot(group_rows, weight_rows, preferred_element_type=jnp.float32).astype(jnp.bfloat16))
        return (running + group_part.astype(jnp.float32), None)
    head_sum, _ = lax.scan(add_group, jnp.zeros((TOKEN_TOTAL, D), jnp.float32), jnp.arange(N_TP, dtype=jnp.int32))
    stream = (residual.astype(jnp.float32) + head_sum).astype(jnp.bfloat16)
    widened = stream.astype(jnp.float32)
    normed = (widened * lax.rsqrt(lax.optimization_barrier(jnp.mean(widened * widened, axis=1, keepdims=True)) + norm_eps) * norm_gain.astype(jnp.float32)).astype(jnp.bfloat16)
    most_rows = N_SP * CAP

    def add_expert(running, expert):
        chosen = routes == expert
        picked_any = jnp.any(chosen, axis=1)
        row_order = jnp.argsort(jnp.where(picked_any, 0, 1).astype(jnp.int32), stable=True)[:most_rows].astype(jnp.int32)
        slot_rows = jnp.take(normed, row_order, axis=0)
        row_share = lax.optimization_barrier(jnp.sum(jnp.where(chosen, route_weight, jnp.zeros_like(route_weight)), axis=1))[row_order]
        gate_value = jnp.dot(slot_rows, gate_weight[expert], preferred_element_type=jnp.float32)
        up_value = jnp.dot(slot_rows, up_weight[expert], preferred_element_type=jnp.float32)
        hidden = (jax.nn.silu(gate_value) * up_value).astype(jnp.bfloat16)
        expert_parts = jnp.einsum('rpf,pfd->prd', hidden.reshape(most_rows, N_TP, FF_PART).astype(jnp.float32), down_weight[expert].reshape(N_TP, FF_PART, D).astype(jnp.float32))
        expert_parts = lax.optimization_barrier(expert_parts.astype(jnp.bfloat16))
        expert_out = lax.optimization_barrier(jnp.sum(expert_parts.astype(jnp.float32), axis=0)).astype(jnp.bfloat16)
        return (running.at[row_order].add(row_share[:, None] * expert_out.astype(jnp.float32)), None)
    mixture, _ = lax.scan(add_expert, jnp.zeros((TOKEN_TOTAL, D), jnp.float32), jnp.arange(EXPERTS, dtype=jnp.int32))
    return (stream.astype(jnp.float32) + mixture).astype(jnp.bfloat16)
```

```python
import functools
import math
import jax
import jax.numpy as jnp
from jax import lax
from jax.experimental import pallas as pl
from jax.experimental.pallas import tpu as pltpu
from jax.sharding import PartitionSpec as P

norm_eps = 1e-06
masked_score = -1e30
key_span = 1024
core_pair = 2
MESH = pl.DeviceIdType.MESH


def remote(src, dst, send_sem, recv_sem, device):
    return pltpu.make_async_remote_copy(
        src_ref=src, dst_ref=dst, send_sem=send_sem, recv_sem=recv_sem,
        device_id=device, device_id_type=MESH,
    )


def greet(sp_count, tp_count):
    me, lane = lax.axis_index("sp"), lax.axis_index("tp")
    barrier = pltpu.get_barrier_semaphore()
    for step in range(1, sp_count):
        pl.semaphore_signal(
            barrier, inc=1, device_id={"sp": lax.rem(me + step, sp_count)}, device_id_type=MESH
        )
    for step in range(1, tp_count):
        pl.semaphore_signal(
            barrier, inc=1, device_id={"tp": lax.rem(lane + step, tp_count)}, device_id_type=MESH
        )
    pl.semaphore_wait(barrier, sp_count + tp_count - 2)


def attend_kernel(
    sp_count, tp_count, q_ref, k_ref, v_ref, c_ref, w_ref, r_ref,
    stream_ref, square_ref,
    q_all, k_all, v_all, c_all, k_rows, c_rows, att_out, att_in, att_rows,
    pa_out, pa_in, pb_out, pb_in, sq_out, sq_in,
    in_send, in_recv, att_send, att_recv, pa_send, pa_recv, pb_send, pb_recv, sq_send, sq_recv,
):
    n = sp_count
    me, lane = lax.axis_index("sp"), lax.axis_index("tp")
    side, row = lax.rem(lane, core_pair), lane // core_pair
    row_count = tp_count // core_pair
    head_width, block = q_ref.shape[1], q_ref.shape[2]
    local_width = r_ref.shape[1]
    partner = {"tp": row * core_pair + (core_pair - 1 - side)}
    greet(sp_count, tp_count)
    pairs = ((k_ref, k_all), (c_ref, c_all), (q_ref, q_all), (v_ref, v_all))
    started = []
    for step in range(1, n):
        peer = lax.rem(me + step, n)
        for kind, (src, dst) in enumerate(pairs):
            copy = remote(
                src.at[peer], dst.at[me], in_send.at[kind, step], in_recv.at[kind, step], {"sp": peer}
            )
            copy.start()
            started.append(copy)
    for src, dst in pairs:
        dst[me] = src[me]
    for copy in started:
        copy.wait()
    scale = head_width ** (-0.5)
    exact = float(math.log2(head_width) / 2).is_integer()
    for j in range(n):
        rows = k_all[j].astype(jnp.float32)
        if exact:
            rows = rows * scale
        k_rows[j * block : (j + 1) * block, :] = rows.T.astype(jnp.bfloat16)
        c_rows[j * block : (j + 1) * block, :] = c_all[j].T
    group = 2 if n % 2 == 0 else 1
    span = group * block

    def one_query(place):
        q = q_all[place]
        cq = c_all[place][0:1, :]
        query_place = place * block + lax.broadcasted_iota(jnp.int32, (span, block), 1)
        key_row = lax.broadcasted_iota(jnp.int32, (span, block), 0)

        def one_key(j, state):
            peak, total, acc = state
            base = pl.multiple_of(j * span, span)
            s = jnp.dot(k_rows[pl.ds(base, span), :], q, preferred_element_type=jnp.float32)
            if not exact:
                s = s * scale
            s = s + (cq - c_rows[pl.ds(base, span), 0:1])
            s = jnp.where(base + key_row <= query_place, s, masked_score)
            new_peak = jnp.maximum(peak, jnp.max(s, axis=0, keepdims=True))
            w = jnp.exp(s - new_peak)
            shrink = jnp.exp(peak - new_peak)
            total = total * shrink + jnp.sum(w, axis=0, keepdims=True)
            wb = w.astype(jnp.bfloat16)
            acc = acc * shrink
            for g in range(group):
                acc = acc + jnp.dot(
                    v_all[j * group + g], wb[g * block : (g + 1) * block, :],
                    preferred_element_type=jnp.float32,
                )
            return new_peak, total, acc

        first = (
            jnp.full((1, block), masked_score, jnp.float32),
            jnp.zeros((1, block), jnp.float32),
            jnp.zeros((head_width, block), jnp.float32),
        )
        peak, total, acc = lax.fori_loop(0, place // group + 1, one_key, first)
        return (acc / total).astype(jnp.bfloat16)

    def send_back(step):
        peer = lax.rem(me + step, n)
        return remote(
            att_out.at[step], att_in.at[me], att_send.at[step], att_recv.at[step], {"sp": peer}
        )

    def one_step(step, carry):
        att_out[step] = one_query(lax.rem(me + step, n))
        send_back(step).start()
        return carry

    lax.fori_loop(1, n, one_step, 0)
    att_in[me] = one_query(me)
    for step in range(1, n):
        send_back(step).wait()
    att_rows[...] = att_in[...].reshape(n * head_width, block).astype(jnp.float32).T.astype(jnp.bfloat16)

    def project(at):
        start = pl.multiple_of(at * local_width, local_width)
        return jnp.dot(
            att_rows[...], w_ref[:, pl.ds(start, local_width)], preferred_element_type=jnp.float32
        )

    across = []
    for r in range(row_count):
        to_row = lax.rem(row + 1 + r, row_count)
        pa_out[r] = project(to_row * core_pair + (core_pair - 1 - side)).astype(jnp.bfloat16)
        copy = remote(pa_out.at[r], pa_in.at[r], pa_send.at[r], pa_recv.at[r], partner)
        copy.start()
        across.append(copy)
    along = []
    for r in range(row_count - 1):
        to_row = lax.rem(row + 1 + r, row_count)
        part = project(to_row * core_pair + side)
        across[r].wait()
        pb_out[r] = (part + pa_in[r].astype(jnp.float32)).astype(jnp.bfloat16)
        copy = remote(
            pb_out.at[r], pb_in.at[r], pb_send.at[r], pb_recv.at[r], {"tp": to_row * core_pair + side}
        )
        copy.start()
        along.append(copy)
    part = project(lane)
    across[row_count - 1].wait()
    part = part + pa_in[row_count - 1].astype(jnp.float32) + r_ref[...].astype(jnp.float32)
    for r in range(row_count - 1):
        along[r].wait()
        part = part + pb_in[r].astype(jnp.float32)
    stream = part.astype(jnp.bfloat16)
    stream_ref[...] = stream
    wide = stream.astype(jnp.float32)
    own = lax.dot_general(
        jnp.ones((8, local_width), jnp.float32), wide * wide, (((1,), (1,)), ((), ())),
        preferred_element_type=jnp.float32, precision=lax.Precision.HIGHEST,
    )
    sq_out[...] = own
    sums = []
    for step in range(1, tp_count):
        copy = remote(
            sq_out, sq_in.at[step], sq_send.at[step], sq_recv.at[step],
            {"tp": lax.rem(lane + step, tp_count)},
        )
        copy.start()
        sums.append(copy)
    for step in range(1, tp_count):
        sums[step - 1].wait()
        own = own + sq_in[step]
    square_ref[...] = own


def dispatch_kernel(
    sp_count, tp_count, t_ref, arr_ref, a_send, a_recv, y_send, y_recv, c_send, c_recv
):
    n = sp_count
    me, lane = lax.axis_index("sp"), lax.axis_index("tp")
    side, row = lax.rem(lane, core_pair), lane // core_pair
    row_count = tp_count // core_pair
    width = t_ref.shape[2]
    partner = {"tp": row * core_pair + (core_pair - 1 - side)}

    def part(source, at):
        return arr_ref.at[source, :, pl.ds(pl.multiple_of(at * width, width), width)]

    greet(sp_count, tp_count)
    entry = [None]
    for step in range(1, n):
        peer = lax.rem(me + step, n)
        copy = remote(t_ref.at[peer], part(me, lane), a_send.at[step], a_recv.at[step], {"sp": peer})
        copy.start()
        entry.append(copy)
    waits, rows = [], []
    for step in range(n):
        source = lax.rem(me + n - step, n)
        if step == 0:
            mine = t_ref.at[me]
        else:
            entry[step].wait()
            mine = part(source, lane)
        if step == 0:
            arr_ref[me, :, pl.ds(pl.multiple_of(lane * width, width), width)] = t_ref[me]
        for r in range(row_count - 1):
            to_row = lax.rem(row + 1 + r, row_count)
            copy = remote(
                mine, part(source, lane), y_send.at[r, step], y_recv.at[r, step],
                {"tp": to_row * core_pair + side},
            )
            copy.start()
            rows.append((r, step, source, copy))
        copy = remote(mine, part(source, lane), c_send.at[0, step], c_recv.at[0, step], partner)
        copy.start()
        waits.append(copy)
    for r, step, source, copy in rows:
        copy.wait()
        from_row = lax.rem(row + row_count - 1 - r, row_count)
        block = part(source, from_row * core_pair + side)
        onward = remote(block, block, c_send.at[1 + r, step], c_recv.at[1 + r, step], partner)
        onward.start()
        waits.append(onward)
    for copy in waits:
        copy.wait()


def collect_kernel(
    sp_count, tp_count, d_ref, back_ref, pa_in, pb_out, pb_in, fin,
    pa_send, pa_recv, pb_send, pb_recv, f_send, f_recv
):
    n = sp_count
    me, lane = lax.axis_index("sp"), lax.axis_index("tp")
    side, row = lax.rem(lane, core_pair), lane // core_pair
    row_count = tp_count // core_pair
    width = back_ref.shape[2]
    partner = {"tp": row * core_pair + (core_pair - 1 - side)}

    def columns(at):
        return pl.ds(pl.multiple_of(at * width, width), width)

    greet(sp_count, tp_count)
    homes = [lax.rem(me + 1 + k, n) for k in range(n)]
    across, along, final = {}, {}, []
    for k in range(n):
        for r in range(row_count):
            to_row = lax.rem(row + 1 + r, row_count)
            at = to_row * core_pair + (core_pair - 1 - side)
            copy = remote(
                d_ref.at[homes[k], :, columns(at)], pa_in.at[r, k],
                pa_send.at[r, k], pa_recv.at[r, k], partner,
            )
            copy.start()
            across[r, k] = copy
    for k in range(n):
        for r in range(row_count - 1):
            at = lax.rem(row + 1 + r, row_count) * core_pair + side
            across[r, k].wait()
            held = d_ref[homes[k], :, columns(at)].astype(jnp.float32)
            pb_out[r, k] = (held + pa_in[r, k].astype(jnp.float32)).astype(jnp.bfloat16)
            copy = remote(
                pb_out.at[r, k], pb_in.at[r, k], pb_send.at[r, k], pb_recv.at[r, k], {"tp": at}
            )
            copy.start()
            along[r, k] = copy
    for k in range(n):
        across[row_count - 1, k].wait()
        total = d_ref[homes[k], :, columns(lane)].astype(jnp.float32)
        total = total + pa_in[row_count - 1, k].astype(jnp.float32)
        for r in range(row_count - 1):
            along[r, k].wait()
            total = total + pb_in[r, k].astype(jnp.float32)
        if k < n - 1:
            fin[k] = total.astype(jnp.bfloat16)
            copy = remote(fin.at[k], back_ref.at[me], f_send.at[k], f_recv.at[k], {"sp": homes[k]})
            copy.start()
            final.append(copy)
        else:
            back_ref[me] = total.astype(jnp.bfloat16)
    for copy in final:
        copy.wait()


def dma(*shape):
    return pltpu.SemaphoreType.DMA(shape)


def vmem_specs(count):
    return [pl.BlockSpec(memory_space=pltpu.VMEM)] * count


def params(number):
    return pltpu.CompilerParams(
        collective_id=number, has_side_effects=True, vmem_limit_bytes=50 * 1024 * 1024
    )


def fast_attention(residual, queries, keys, values, forget_cache, out_weight, sp_count, tp_count):
    token_count, local_width = residual.shape
    head_count = forget_cache.shape[0]
    head_width = queries.shape[0] // head_count
    heads = (head_count, head_width, token_count)
    cache = jnp.broadcast_to(forget_cache[:, None, :], (head_count, 8, token_count))
    row_count = tp_count // core_pair
    half, full = jnp.bfloat16, jnp.float32
    block = (token_count, local_width)
    return pl.pallas_call(
        functools.partial(attend_kernel, sp_count, tp_count),
        out_shape=(
            jax.ShapeDtypeStruct(block, half),
            jax.ShapeDtypeStruct((8, token_count), full),
        ),
        in_specs=vmem_specs(6),
        out_specs=tuple(vmem_specs(2)),
        scratch_shapes=[
            pltpu.VMEM(heads, half),
            pltpu.VMEM(heads, half),
            pltpu.VMEM(heads, half),
            pltpu.VMEM((sp_count, 8, token_count), full),
            pltpu.VMEM((sp_count * token_count, head_width), half),
            pltpu.VMEM((sp_count * token_count, 8), full),
            pltpu.VMEM(heads, half),
            pltpu.VMEM(heads, half),
            pltpu.VMEM((token_count, head_count * head_width), half),
            pltpu.VMEM((row_count,) + block, half),
            pltpu.VMEM((row_count,) + block, half),
            pltpu.VMEM((row_count,) + block, half),
            pltpu.VMEM((row_count,) + block, half),
            pltpu.VMEM((8, token_count), full),
            pltpu.VMEM((tp_count, 8, token_count), full),
            dma(4, sp_count), dma(4, sp_count), dma(sp_count), dma(sp_count),
            dma(row_count), dma(row_count), dma(row_count), dma(row_count),
            dma(tp_count), dma(tp_count),
        ],
        compiler_params=params(0),
    )(queries.reshape(heads), keys.reshape(heads), values.reshape(heads), cache, out_weight, residual)


def fast_dispatch(taken, sp_count, tp_count, model_width):
    capacity = taken.shape[1]
    row_count = tp_count // core_pair
    return pl.pallas_call(
        functools.partial(dispatch_kernel, sp_count, tp_count),
        out_shape=jax.ShapeDtypeStruct((sp_count, capacity, model_width), jnp.bfloat16),
        in_specs=vmem_specs(1),
        out_specs=vmem_specs(1)[0],
        scratch_shapes=[
            dma(sp_count), dma(sp_count), dma(row_count, sp_count), dma(row_count, sp_count),
            dma(row_count, sp_count), dma(row_count, sp_count),
        ],
        compiler_params=params(1),
    )(taken)


def fast_collect(down, sp_count, tp_count):
    capacity, local_width = down.shape[1], down.shape[2] // tp_count
    row_count = tp_count // core_pair
    piece = (sp_count, capacity, local_width)
    half = jnp.bfloat16
    return pl.pallas_call(
        functools.partial(collect_kernel, sp_count, tp_count),
        out_shape=jax.ShapeDtypeStruct(piece, half),
        in_specs=vmem_specs(1),
        out_specs=vmem_specs(1)[0],
        scratch_shapes=[
            pltpu.VMEM((row_count,) + piece, half),
            pltpu.VMEM((row_count,) + piece, half),
            pltpu.VMEM((row_count,) + piece, half),
            pltpu.VMEM(piece, half),
            dma(row_count, sp_count), dma(row_count, sp_count),
            dma(row_count, sp_count), dma(row_count, sp_count),
            dma(sp_count), dma(sp_count),
        ],
        compiler_params=params(2),
    )(down)


def ring_attention(
    residual,
    queries,
    keys,
    values,
    forget_cache,
    out_weight,
):
    sp_count = lax.axis_size("sp")
    token_count = residual.shape[0]
    head_count = forget_cache.shape[0]
    head_width = queries.shape[0] // head_count
    first_token = lax.axis_index("sp") * token_count
    last_token = first_token + token_count - 1
    query_heads = queries.reshape(head_count, head_width, token_count)
    query_place = first_token + jnp.arange(token_count, dtype=jnp.int32)
    score_scale = head_width ** (-0.5)

    def attend_block(state_now, key_block, value_block, cache_block, key_first):
        running_peak, running_total, running_sum = state_now
        block_length = key_block.shape[1]
        key_heads = key_block.reshape(head_count, head_width, block_length)
        value_heads = value_block.reshape(head_count, head_width, block_length)
        scores = (
            jnp.einsum("hdq,hdk->hqk", query_heads, key_heads, preferred_element_type=jnp.float32)
            * score_scale
        )
        scores = scores + forget_cache[:, :, None] - cache_block[:, None, :]
        key_place = key_first + jnp.arange(block_length, dtype=jnp.int32)
        allowed = key_place[None, :] <= query_place[:, None]
        scores = jnp.where(allowed[None], scores, masked_score)
        new_peak = jnp.maximum(running_peak, jnp.max(scores, axis=2))
        weights = jnp.exp(scores - new_peak[:, :, None])
        shrink = jnp.exp(running_peak - new_peak)
        new_total = running_total * shrink + jnp.sum(weights, axis=2)
        new_sum = running_sum * shrink[:, None, :] + jnp.einsum(
            "hdk,hqk->hdq",
            value_heads,
            weights.astype(jnp.bfloat16),
            preferred_element_type=jnp.float32,
        )
        return (new_peak, new_total, new_sum)

    initial = (
        jnp.full((head_count, token_count), masked_score, jnp.float32),
        jnp.zeros((head_count, token_count), jnp.float32),
        jnp.zeros((head_count, head_width, token_count), jnp.float32),
    )
    key_part = lax.all_gather(keys.astype(jnp.float32), "sp", axis=1, tiled=True).astype(
        jnp.bfloat16
    )
    value_part = lax.all_gather(values.astype(jnp.float32), "sp", axis=1, tiled=True).astype(
        jnp.bfloat16
    )
    cache_part = lax.all_gather(forget_cache, "sp", axis=1, tiled=True)
    part_length = key_part.shape[1]
    block_length = key_span

    def one_block(block_index, state_in):
        start_column = block_index * block_length
        key_block = lax.dynamic_slice_in_dim(key_part, start_column, block_length, 1)
        value_block = lax.dynamic_slice_in_dim(value_part, start_column, block_length, 1)
        cache_block = lax.dynamic_slice_in_dim(cache_part, start_column, block_length, 1)
        return lax.cond(
            start_column <= last_token,
            lambda inner: attend_block(inner, key_block, value_block, cache_block, start_column),
            lambda inner: inner,
            state_in,
        )

    final_peak, final_total, final_sum = lax.fori_loop(
        0, part_length // block_length, one_block, initial
    )
    attended = (
        (final_sum / final_total[:, None, :])
        .astype(jnp.bfloat16)
        .reshape(head_count * head_width, token_count)
    )
    projected = lax.dot_general(
        attended, out_weight, (((0,), (0,)), ((), ())), preferred_element_type=jnp.float32
    )
    head_sum = lax.psum_scatter(
        projected.astype(jnp.bfloat16), "tp", scatter_dimension=1, tiled=True
    ).astype(jnp.float32)
    stream = (residual.astype(jnp.float32) + head_sum).astype(jnp.bfloat16)
    local_rows = stream.astype(jnp.float32)
    return stream, lax.psum(jnp.sum(local_rows * local_rows, axis=1), "tp")


def shards(
    residual,
    queries,
    keys,
    values,
    forget_cache,
    out_weight,
    norm_gain,
    routes,
    route_weight,
    gate_weight,
    up_weight,
    down_weight,
):
    sp_count, tp_count = lax.axis_size("sp"), lax.axis_size("tp")
    token_count, local_width = residual.shape
    model_width = norm_gain.shape[0]
    top_count = routes.shape[1]
    item_count = token_count * top_count
    capacity = max(2, token_count * top_count * 5 // (4 * sp_count))
    slot_total = sp_count * capacity
    paired = tp_count % core_pair == 0 and tp_count > core_pair and local_width % 128 == 0
    head_count = forget_cache.shape[0]
    if paired and head_count == sp_count:
        stream, squares = fast_attention(
            residual, queries, keys, values, forget_cache, out_weight, sp_count, tp_count
        )
        squares = squares[0]
    else:
        stream, squares = ring_attention(residual, queries, keys, values, forget_cache, out_weight)
    local_rows = stream.astype(jnp.float32)
    expert_of = routes.reshape(item_count)
    onehot = (expert_of[:, None] == jnp.arange(sp_count, dtype=jnp.int32)[None, :]).astype(
        jnp.int32
    )
    earlier = jnp.cumsum(onehot, axis=0) - onehot
    target = (expert_of * capacity + jnp.sum(earlier * onehot, axis=1)).reshape(
        token_count, top_count
    )
    slots = jnp.arange(slot_total, dtype=jnp.int32)
    row_scale = lax.rsqrt(squares / model_width + norm_eps)
    local_gain = lax.dynamic_slice_in_dim(
        norm_gain, lax.axis_index("tp") * local_width, local_width
    )
    normed = (local_rows * row_scale[:, None] * local_gain[None, :]).astype(jnp.bfloat16)
    pick = jnp.any(target.T[:, None, :] == slots[None, :, None], axis=0).astype(jnp.bfloat16)
    taken_rows = (
        jnp.dot(pick, normed, preferred_element_type=jnp.float32)
        .astype(jnp.bfloat16)
        .reshape(sp_count, capacity, local_width)
    )
    direct = paired and capacity % 16 == 0
    if direct:
        arrived = fast_dispatch(taken_rows, sp_count, tp_count, model_width)
    else:
        arrived = lax.all_gather(
            lax.all_to_all(taken_rows, "sp", split_axis=0, concat_axis=0, tiled=True),
            "tp",
            axis=2,
            tiled=True,
        )
    flat_rows = arrived.reshape(slot_total, model_width)
    gate_value = jnp.dot(flat_rows, gate_weight[0], preferred_element_type=jnp.float32)
    up_value = jnp.dot(flat_rows, up_weight[0], preferred_element_type=jnp.float32)
    hidden = (jax.nn.silu(gate_value) * up_value).astype(jnp.bfloat16)
    down_value = (
        jnp.dot(hidden, down_weight[0], preferred_element_type=jnp.float32)
        .astype(jnp.bfloat16)
        .reshape(sp_count, capacity, model_width)
    )
    if direct:
        expert_back = fast_collect(down_value, sp_count, tp_count)
    else:
        summed = lax.psum_scatter(down_value, "tp", scatter_dimension=2, tiled=True)
        expert_back = lax.all_to_all(summed, "sp", split_axis=0, concat_axis=0, tiled=True)
    back_rows = expert_back.reshape(slot_total, local_width)
    share = jnp.sum(
        jnp.where(target[:, :, None] == slots[None, None, :], route_weight[:, :, None], 0.0), axis=1
    )
    share_high = share.astype(jnp.bfloat16)
    share_low = (share - share_high.astype(jnp.float32)).astype(jnp.bfloat16)
    mixture = jnp.dot(share_high, back_rows, preferred_element_type=jnp.float32) + jnp.dot(
        share_low, back_rows, preferred_element_type=jnp.float32
    )
    return (local_rows + mixture).astype(jnp.bfloat16)


def solution(mesh):
    return jax.shard_map(
        shards,
        mesh=mesh,
        in_specs=(
            P("sp", "tp"),
            P("tp", "sp"),
            P("tp", "sp"),
            P("tp", "sp"),
            P("tp", "sp"),
            P("tp", None),
            P(),
            P("sp", None),
            P("sp", None),
            P("sp", None, "tp"),
            P("sp", None, "tp"),
            P("sp", "tp", None),
        ),
        out_specs=P("sp", "tp"),
        check_vma=False,
    )
```

```python
import functools
import math
import jax
import jax.numpy as jnp
from jax import lax
from jax.experimental import pallas as pl
from jax.experimental.pallas import tpu as pltpu
from jax.sharding import PartitionSpec as P

norm_eps = 1e-06
masked_score = -1e30
key_span = 1024
core_pair = 2
MESH = pl.DeviceIdType.MESH


def remote(src, dst, send_sem, recv_sem, device):
    return pltpu.make_async_remote_copy(
        src_ref=src, dst_ref=dst, send_sem=send_sem, recv_sem=recv_sem,
        device_id=device, device_id_type=MESH,
    )


def greet(sp_count, tp_count):
    me, lane = lax.axis_index("sp"), lax.axis_index("tp")
    barrier = pltpu.get_barrier_semaphore()
    for step in range(1, sp_count):
        pl.semaphore_signal(
            barrier, inc=1, device_id={"sp": lax.rem(me + step, sp_count)}, device_id_type=MESH
        )
    for step in range(1, tp_count):
        pl.semaphore_signal(
            barrier, inc=1, device_id={"tp": lax.rem(lane + step, tp_count)}, device_id_type=MESH
        )
    pl.semaphore_wait(barrier, sp_count + tp_count - 2)


def attend_kernel(
    sp_count, tp_count, q_hbm, k_hbm, v_hbm, c_ref, w_hbm, r_hbm,
    stream_ref, square_ref,
    q_ref, k_ref, v_ref, w_ref, r_ref, load_sem,
    q_all, k_all, v_all, c_all, k_rows, c_rows, att_out, att_in, att_rows,
    pa_out, pa_in, pb_out, pb_in, sq_out, sq_in,
    in_send, in_recv, att_send, att_recv, pa_send, pa_recv, pb_send, pb_recv, sq_send, sq_recv,
):
    n = sp_count
    me, lane = lax.axis_index("sp"), lax.axis_index("tp")
    side, row = lax.rem(lane, core_pair), lane // core_pair
    row_count = tp_count // core_pair
    head_width, block = q_ref.shape[1], q_ref.shape[2]
    local_width = r_ref.shape[1]
    partner = {"tp": row * core_pair + (core_pair - 1 - side)}
    loads = []
    for at, (src, dst) in enumerate(
        ((k_hbm, k_ref), (q_hbm, q_ref), (v_hbm, v_ref), (w_hbm, w_ref), (r_hbm, r_ref))
    ):
        loads.append(pltpu.make_async_copy(src, dst, load_sem.at[at]))
        loads[at].start()
    greet(sp_count, tp_count)
    for at in range(3):
        loads[at].wait()
    pairs = ((k_ref, k_all), (c_ref, c_all), (q_ref, q_all), (v_ref, v_all))
    started = []
    for step in range(1, n):
        peer = lax.rem(me + step, n)
        for kind, (src, dst) in enumerate(pairs):
            copy = remote(
                src.at[peer], dst.at[me], in_send.at[kind, step], in_recv.at[kind, step], {"sp": peer}
            )
            copy.start()
            started.append(copy)
    for src, dst in pairs:
        dst[me] = src[me]
    for copy in started:
        copy.wait()
    scale = head_width ** (-0.5)
    exact = float(math.log2(head_width) / 2).is_integer()
    for j in range(n):
        rows = k_all[j].astype(jnp.float32)
        if exact:
            rows = rows * scale
        k_rows[j * block : (j + 1) * block, :] = rows.T.astype(jnp.bfloat16)
        c_rows[j * block : (j + 1) * block, :] = c_all[j].T
    group = 2 if n % 2 == 0 else 1
    span = group * block

    def one_query(place):
        q = q_all[place]
        cq = c_all[place][0:1, :]
        query_place = place * block + lax.broadcasted_iota(jnp.int32, (span, block), 1)
        key_row = lax.broadcasted_iota(jnp.int32, (span, block), 0)

        def one_key(j, state):
            peak, total, acc = state
            base = pl.multiple_of(j * span, span)
            s = jnp.dot(k_rows[pl.ds(base, span), :], q, preferred_element_type=jnp.float32)
            if not exact:
                s = s * scale
            s = s + (cq - c_rows[pl.ds(base, span), 0:1])
            s = jnp.where(base + key_row <= query_place, s, masked_score)
            new_peak = jnp.maximum(peak, jnp.max(s, axis=0, keepdims=True))
            w = jnp.exp(s - new_peak)
            shrink = jnp.exp(peak - new_peak)
            total = total * shrink + jnp.sum(w, axis=0, keepdims=True)
            wb = w.astype(jnp.bfloat16)
            acc = acc * shrink
            for g in range(group):
                acc = acc + jnp.dot(
                    v_all[j * group + g], wb[g * block : (g + 1) * block, :],
                    preferred_element_type=jnp.float32,
                )
            return new_peak, total, acc

        first = (
            jnp.full((1, block), masked_score, jnp.float32),
            jnp.zeros((1, block), jnp.float32),
            jnp.zeros((head_width, block), jnp.float32),
        )
        peak, total, acc = lax.fori_loop(0, place // group + 1, one_key, first)
        return (acc / total).astype(jnp.bfloat16)

    def send_back(step):
        peer = lax.rem(me + step, n)
        return remote(
            att_out.at[step], att_in.at[me], att_send.at[step], att_recv.at[step], {"sp": peer}
        )

    def one_step(step, carry):
        att_out[step] = one_query(lax.rem(me + step, n))
        send_back(step).start()
        return carry

    lax.fori_loop(1, n, one_step, 0)
    att_in[me] = one_query(me)
    for step in range(1, n):
        send_back(step).wait()
    att_rows[...] = att_in[...].reshape(n * head_width, block).astype(jnp.float32).T.astype(jnp.bfloat16)

    for at in range(3, 5):
        loads[at].wait()

    def project(at):
        start = pl.multiple_of(at * local_width, local_width)
        return jnp.dot(
            att_rows[...], w_ref[:, pl.ds(start, local_width)], preferred_element_type=jnp.float32
        )

    across = []
    for r in range(row_count):
        to_row = lax.rem(row + 1 + r, row_count)
        pa_out[r] = project(to_row * core_pair + (core_pair - 1 - side)).astype(jnp.bfloat16)
        copy = remote(pa_out.at[r], pa_in.at[r], pa_send.at[r], pa_recv.at[r], partner)
        copy.start()
        across.append(copy)
    along = []
    for r in range(row_count - 1):
        to_row = lax.rem(row + 1 + r, row_count)
        part = project(to_row * core_pair + side)
        across[r].wait()
        pb_out[r] = (part + pa_in[r].astype(jnp.float32)).astype(jnp.bfloat16)
        copy = remote(
            pb_out.at[r], pb_in.at[r], pb_send.at[r], pb_recv.at[r], {"tp": to_row * core_pair + side}
        )
        copy.start()
        along.append(copy)
    part = project(lane)
    across[row_count - 1].wait()
    part = part + pa_in[row_count - 1].astype(jnp.float32) + r_ref[...].astype(jnp.float32)
    for r in range(row_count - 1):
        along[r].wait()
        part = part + pb_in[r].astype(jnp.float32)
    stream = part.astype(jnp.bfloat16)
    stream_ref[...] = stream
    wide = stream.astype(jnp.float32)
    own = lax.dot_general(
        jnp.ones((8, local_width), jnp.float32), wide * wide, (((1,), (1,)), ((), ())),
        preferred_element_type=jnp.float32, precision=lax.Precision.HIGHEST,
    )
    sq_out[...] = own
    sums = []
    for step in range(1, tp_count):
        copy = remote(
            sq_out, sq_in.at[step], sq_send.at[step], sq_recv.at[step],
            {"tp": lax.rem(lane + step, tp_count)},
        )
        copy.start()
        sums.append(copy)
    for step in range(1, tp_count):
        sums[step - 1].wait()
        own = own + sq_in[step]
    square_ref[...] = own


def expert_kernel(
    sp_count, tp_count, t_ref, g_hbm, u_hbm, d_hbm, back_ref,
    g_ref, u_ref, d_ref, arr, hid, down, pa_in, pb_out, pb_in, fin,
    load_sem, a_send, a_recv, y_send, y_recv, c_send, c_recv,
    pa_send, pa_recv, pb_send, pb_recv, f_send, f_recv
):
    n = sp_count
    me, lane = lax.axis_index("sp"), lax.axis_index("tp")
    side, row = lax.rem(lane, core_pair), lane // core_pair
    row_count = tp_count // core_pair
    capacity, width = t_ref.shape[1], t_ref.shape[2]
    model_width, hidden_width = g_ref.shape
    partner = {"tp": row * core_pair + (core_pair - 1 - side)}
    loads = []
    for at, (src, dst) in enumerate(((g_hbm, g_ref), (u_hbm, u_ref), (d_hbm, d_ref))):
        loads.append(pltpu.make_async_copy(src.at[0], dst, load_sem.at[at]))
        loads[at].start()

    def columns(at):
        return pl.ds(pl.multiple_of(at * width, width), width)

    def part(step, at):
        return arr.at[step, :, columns(at)]

    greet(sp_count, tp_count)
    entry = [None]
    for step in range(1, n):
        peer = lax.rem(me + step, n)
        copy = remote(t_ref.at[peer], part(step, lane), a_send.at[step], a_recv.at[step], {"sp": peer})
        copy.start()
        entry.append(copy)
    homes = [lax.rem(me + n - k, n) for k in range(n)]
    sides, rows, across, along, final = {}, {}, {}, {}, []

    def forward(step):
        if step == 0:
            arr[0, :, columns(lane)] = t_ref[me]
            mine = t_ref.at[me]
        else:
            entry[step].wait()
            mine = part(step, lane)
        for r in range(row_count - 1):
            to_row = lax.rem(row + 1 + r, row_count)
            rows[r, step] = remote(
                mine, part(step, lane), y_send.at[r, step], y_recv.at[r, step],
                {"tp": to_row * core_pair + side},
            )
            rows[r, step].start()
        sides[0, step] = remote(
            mine, part(step, lane), c_send.at[0, step], c_recv.at[0, step], partner
        )
        sides[0, step].start()

    def relay(step):
        for r in range(row_count - 1):
            rows[r, step].wait()
            from_row = lax.rem(row + row_count - 1 - r, row_count)
            block = part(step, from_row * core_pair + side)
            sides[1 + r, step] = remote(
                block, block, c_send.at[1 + r, step], c_recv.at[1 + r, step], partner
            )
            sides[1 + r, step].start()

    def tile_of(total):
        return 256 if total % 256 == 0 else 128

    hidden_tile, down_tile = tile_of(hidden_width), tile_of(model_width)

    def compute(first, count):
        for step in range(first, first + count):
            for r in range(row_count):
                sides[r, step].wait()
        height = count * capacity
        if first == 0:
            for load in loads:
                load.wait()

        def one_hidden(f, carry):
            at = pl.ds(pl.multiple_of(f * hidden_tile, hidden_tile), hidden_tile)
            x = arr[first : first + count].reshape(height, model_width)
            gate = jnp.dot(x, g_ref[:, at], preferred_element_type=jnp.float32)
            up = jnp.dot(x, u_ref[:, at], preferred_element_type=jnp.float32)
            value = (gate / (1.0 + jnp.exp(-gate))) * up
            hid[0:height, at] = value.astype(jnp.bfloat16)
            return carry

        lax.fori_loop(0, hidden_width // hidden_tile, one_hidden, 0)

        def one_down(f, carry):
            at = pl.ds(pl.multiple_of(f * down_tile, down_tile), down_tile)
            value = jnp.dot(hid[0:height, :], d_ref[:, at], preferred_element_type=jnp.float32)
            down[first : first + count, :, at] = value.astype(jnp.bfloat16).reshape(
                count, capacity, down_tile
            )
            return carry

        lax.fori_loop(0, model_width // down_tile, one_down, 0)
        for k in range(first, first + count):
            for r in range(row_count):
                to_row = lax.rem(row + 1 + r, row_count)
                at = to_row * core_pair + (core_pair - 1 - side)
                across[r, k] = remote(
                    down.at[k, :, columns(at)], pa_in.at[r, k],
                    pa_send.at[r, k], pa_recv.at[r, k], partner,
                )
                across[r, k].start()

    def exchange(k):
        for r in range(row_count - 1):
            at = lax.rem(row + 1 + r, row_count) * core_pair + side
            across[r, k].wait()
            held = down[k, :, columns(at)].astype(jnp.float32)
            pb_out[r, k] = (held + pa_in[r, k].astype(jnp.float32)).astype(jnp.bfloat16)
            along[r, k] = remote(
                pb_out.at[r, k], pb_in.at[r, k], pb_send.at[r, k], pb_recv.at[r, k], {"tp": at}
            )
            along[r, k].start()

    def finish(k):
        across[row_count - 1, k].wait()
        total = down[k, :, columns(lane)].astype(jnp.float32)
        total = total + pa_in[row_count - 1, k].astype(jnp.float32)
        for r in range(row_count - 1):
            along[r, k].wait()
            total = total + pb_in[r, k].astype(jnp.float32)
        if k > 0:
            fin[k] = total.astype(jnp.bfloat16)
            copy = remote(fin.at[k], back_ref.at[me], f_send.at[k], f_recv.at[k], {"sp": homes[k]})
            copy.start()
            final.append(copy)
        else:
            back_ref[me] = total.astype(jnp.bfloat16)

    count = 2 if n % 2 == 0 else 1
    groups = n // count
    for g in range(groups + 4):
        for stage in range(5):
            at = g - stage
            if not 0 <= at < groups:
                continue
            if stage == 2:
                compute(at * count, count)
                continue
            for step in range(at * count, at * count + count):
                (forward, relay, None, exchange, finish)[stage](step)
    for copy in final:
        copy.wait()


def dma(*shape):
    return pltpu.SemaphoreType.DMA(shape)


def vmem_specs(count):
    return [pl.BlockSpec(memory_space=pltpu.VMEM)] * count


def hbm_specs(count):
    return [pl.BlockSpec(memory_space=pltpu.HBM)] * count


def params(number):
    return pltpu.CompilerParams(
        collective_id=number, has_side_effects=True, vmem_limit_bytes=50 * 1024 * 1024
    )


def fast_attention(residual, queries, keys, values, forget_cache, out_weight, sp_count, tp_count):
    token_count, local_width = residual.shape
    head_count = forget_cache.shape[0]
    head_width = queries.shape[0] // head_count
    heads = (head_count, head_width, token_count)
    cache = jnp.broadcast_to(forget_cache[:, None, :], (head_count, 8, token_count))
    row_count = tp_count // core_pair
    half, full = jnp.bfloat16, jnp.float32
    block = (token_count, local_width)
    return pl.pallas_call(
        functools.partial(attend_kernel, sp_count, tp_count),
        out_shape=(
            jax.ShapeDtypeStruct(block, half),
            jax.ShapeDtypeStruct((8, token_count), full),
        ),
        in_specs=hbm_specs(3) + vmem_specs(1) + hbm_specs(2),
        out_specs=tuple(vmem_specs(2)),
        scratch_shapes=[
            pltpu.VMEM(heads, half),
            pltpu.VMEM(heads, half),
            pltpu.VMEM(heads, half),
            pltpu.VMEM(out_weight.shape, half),
            pltpu.VMEM(block, half),
            dma(5),
            pltpu.VMEM(heads, half),
            pltpu.VMEM(heads, half),
            pltpu.VMEM(heads, half),
            pltpu.VMEM((sp_count, 8, token_count), full),
            pltpu.VMEM((sp_count * token_count, head_width), half),
            pltpu.VMEM((sp_count * token_count, 8), full),
            pltpu.VMEM(heads, half),
            pltpu.VMEM(heads, half),
            pltpu.VMEM((token_count, head_count * head_width), half),
            pltpu.VMEM((row_count,) + block, half),
            pltpu.VMEM((row_count,) + block, half),
            pltpu.VMEM((row_count,) + block, half),
            pltpu.VMEM((row_count,) + block, half),
            pltpu.VMEM((8, token_count), full),
            pltpu.VMEM((tp_count, 8, token_count), full),
            dma(4, sp_count), dma(4, sp_count), dma(sp_count), dma(sp_count),
            dma(row_count), dma(row_count), dma(row_count), dma(row_count),
            dma(tp_count), dma(tp_count),
        ],
        compiler_params=params(0),
    )(queries.reshape(heads), keys.reshape(heads), values.reshape(heads), cache, out_weight, residual)


def fast_experts(taken, gate_weight, up_weight, down_weight, sp_count, tp_count):
    piece = taken.shape
    capacity = piece[1]
    model_width, hidden_width = gate_weight.shape[1:]
    row_count = tp_count // core_pair
    half = jnp.bfloat16
    wide = (sp_count, capacity, model_width)
    pairs = (row_count, sp_count)
    return pl.pallas_call(
        functools.partial(expert_kernel, sp_count, tp_count),
        out_shape=jax.ShapeDtypeStruct(piece, half),
        in_specs=vmem_specs(1) + hbm_specs(3),
        out_specs=vmem_specs(1)[0],
        scratch_shapes=[
            pltpu.VMEM(gate_weight.shape[1:], half),
            pltpu.VMEM(up_weight.shape[1:], half),
            pltpu.VMEM(down_weight.shape[1:], half),
            pltpu.VMEM(wide, half),
            pltpu.VMEM((2 * capacity, hidden_width), half),
            pltpu.VMEM(wide, half),
            pltpu.VMEM((row_count,) + piece, half),
            pltpu.VMEM((row_count,) + piece, half),
            pltpu.VMEM((row_count,) + piece, half),
            pltpu.VMEM(piece, half),
            dma(3), dma(sp_count), dma(sp_count),
            dma(*pairs), dma(*pairs), dma(*pairs), dma(*pairs),
            dma(*pairs), dma(*pairs), dma(*pairs), dma(*pairs),
            dma(sp_count), dma(sp_count),
        ],
        compiler_params=params(1),
    )(taken, gate_weight, up_weight, down_weight)


def ring_attention(
    residual,
    queries,
    keys,
    values,
    forget_cache,
    out_weight,
):
    sp_count = lax.axis_size("sp")
    token_count = residual.shape[0]
    head_count = forget_cache.shape[0]
    head_width = queries.shape[0] // head_count
    first_token = lax.axis_index("sp") * token_count
    last_token = first_token + token_count - 1
    query_heads = queries.reshape(head_count, head_width, token_count)
    query_place = first_token + jnp.arange(token_count, dtype=jnp.int32)
    score_scale = head_width ** (-0.5)

    def attend_block(state_now, key_block, value_block, cache_block, key_first):
        running_peak, running_total, running_sum = state_now
        block_length = key_block.shape[1]
        key_heads = key_block.reshape(head_count, head_width, block_length)
        value_heads = value_block.reshape(head_count, head_width, block_length)
        scores = (
            jnp.einsum("hdq,hdk->hqk", query_heads, key_heads, preferred_element_type=jnp.float32)
            * score_scale
        )
        scores = scores + forget_cache[:, :, None] - cache_block[:, None, :]
        key_place = key_first + jnp.arange(block_length, dtype=jnp.int32)
        allowed = key_place[None, :] <= query_place[:, None]
        scores = jnp.where(allowed[None], scores, masked_score)
        new_peak = jnp.maximum(running_peak, jnp.max(scores, axis=2))
        weights = jnp.exp(scores - new_peak[:, :, None])
        shrink = jnp.exp(running_peak - new_peak)
        new_total = running_total * shrink + jnp.sum(weights, axis=2)
        new_sum = running_sum * shrink[:, None, :] + jnp.einsum(
            "hdk,hqk->hdq",
            value_heads,
            weights.astype(jnp.bfloat16),
            preferred_element_type=jnp.float32,
        )
        return (new_peak, new_total, new_sum)

    initial = (
        jnp.full((head_count, token_count), masked_score, jnp.float32),
        jnp.zeros((head_count, token_count), jnp.float32),
        jnp.zeros((head_count, head_width, token_count), jnp.float32),
    )
    key_part = lax.all_gather(keys.astype(jnp.float32), "sp", axis=1, tiled=True).astype(
        jnp.bfloat16
    )
    value_part = lax.all_gather(values.astype(jnp.float32), "sp", axis=1, tiled=True).astype(
        jnp.bfloat16
    )
    cache_part = lax.all_gather(forget_cache, "sp", axis=1, tiled=True)
    part_length = key_part.shape[1]
    block_length = key_span

    def one_block(block_index, state_in):
        start_column = block_index * block_length
        key_block = lax.dynamic_slice_in_dim(key_part, start_column, block_length, 1)
        value_block = lax.dynamic_slice_in_dim(value_part, start_column, block_length, 1)
        cache_block = lax.dynamic_slice_in_dim(cache_part, start_column, block_length, 1)
        return lax.cond(
            start_column <= last_token,
            lambda inner: attend_block(inner, key_block, value_block, cache_block, start_column),
            lambda inner: inner,
            state_in,
        )

    final_peak, final_total, final_sum = lax.fori_loop(
        0, part_length // block_length, one_block, initial
    )
    attended = (
        (final_sum / final_total[:, None, :])
        .astype(jnp.bfloat16)
        .reshape(head_count * head_width, token_count)
    )
    projected = lax.dot_general(
        attended, out_weight, (((0,), (0,)), ((), ())), preferred_element_type=jnp.float32
    )
    head_sum = lax.psum_scatter(
        projected.astype(jnp.bfloat16), "tp", scatter_dimension=1, tiled=True
    ).astype(jnp.float32)
    stream = (residual.astype(jnp.float32) + head_sum).astype(jnp.bfloat16)
    local_rows = stream.astype(jnp.float32)
    return stream, lax.psum(jnp.sum(local_rows * local_rows, axis=1), "tp")


def shards(
    residual,
    queries,
    keys,
    values,
    forget_cache,
    out_weight,
    norm_gain,
    routes,
    route_weight,
    gate_weight,
    up_weight,
    down_weight,
):
    sp_count, tp_count = lax.axis_size("sp"), lax.axis_size("tp")
    token_count, local_width = residual.shape
    model_width = norm_gain.shape[0]
    top_count = routes.shape[1]
    item_count = token_count * top_count
    capacity = max(2, token_count * top_count * 5 // (4 * sp_count))
    slot_total = sp_count * capacity
    paired = tp_count % core_pair == 0 and tp_count > core_pair and local_width % 128 == 0
    head_count = forget_cache.shape[0]
    if paired and head_count == sp_count:
        stream, squares = fast_attention(
            residual, queries, keys, values, forget_cache, out_weight, sp_count, tp_count
        )
        squares = squares[0]
    else:
        stream, squares = ring_attention(residual, queries, keys, values, forget_cache, out_weight)
    local_rows = stream.astype(jnp.float32)
    expert_of = routes.reshape(item_count)
    onehot = (expert_of[:, None] == jnp.arange(sp_count, dtype=jnp.int32)[None, :]).astype(
        jnp.int32
    )
    earlier = jnp.cumsum(onehot, axis=0) - onehot
    target = (expert_of * capacity + jnp.sum(earlier * onehot, axis=1)).reshape(
        token_count, top_count
    )
    slots = jnp.arange(slot_total, dtype=jnp.int32)
    row_scale = lax.rsqrt(squares / model_width + norm_eps)
    local_gain = lax.dynamic_slice_in_dim(
        norm_gain, lax.axis_index("tp") * local_width, local_width
    )
    normed = (local_rows * row_scale[:, None] * local_gain[None, :]).astype(jnp.bfloat16)
    pick = jnp.any(target.T[:, None, :] == slots[None, :, None], axis=0).astype(jnp.bfloat16)
    taken_rows = (
        jnp.dot(pick, normed, preferred_element_type=jnp.float32)
        .astype(jnp.bfloat16)
        .reshape(sp_count, capacity, local_width)
    )
    if paired and capacity % 16 == 0:
        expert_back = fast_experts(
            taken_rows, gate_weight, up_weight, down_weight, sp_count, tp_count
        )
    else:
        arrived = lax.all_gather(
            lax.all_to_all(taken_rows, "sp", split_axis=0, concat_axis=0, tiled=True),
            "tp",
            axis=2,
            tiled=True,
        )
        flat_rows = arrived.reshape(slot_total, model_width)
        gate_value = jnp.dot(flat_rows, gate_weight[0], preferred_element_type=jnp.float32)
        up_value = jnp.dot(flat_rows, up_weight[0], preferred_element_type=jnp.float32)
        hidden = (jax.nn.silu(gate_value) * up_value).astype(jnp.bfloat16)
        down_value = jnp.dot(hidden, down_weight[0], preferred_element_type=jnp.float32)
        summed = lax.psum_scatter(
            down_value.reshape(sp_count, capacity, model_width).astype(jnp.bfloat16),
            "tp",
            scatter_dimension=2,
            tiled=True,
        )
        expert_back = lax.all_to_all(summed, "sp", split_axis=0, concat_axis=0, tiled=True)
    back_rows = expert_back.reshape(slot_total, local_width)
    share = jnp.sum(
        jnp.where(target[:, :, None] == slots[None, None, :], route_weight[:, :, None], 0.0), axis=1
    )
    share_high = share.astype(jnp.bfloat16)
    share_low = (share - share_high.astype(jnp.float32)).astype(jnp.bfloat16)
    mixture = jnp.dot(share_high, back_rows, preferred_element_type=jnp.float32) + jnp.dot(
        share_low, back_rows, preferred_element_type=jnp.float32
    )
    return (local_rows + mixture).astype(jnp.bfloat16)


def solution(mesh):
    return jax.shard_map(
        shards,
        mesh=mesh,
        in_specs=(
            P("sp", "tp"),
            P("tp", "sp"),
            P("tp", "sp"),
            P("tp", "sp"),
            P("tp", "sp"),
            P("tp", None),
            P(),
            P("sp", None),
            P("sp", None),
            P("sp", None, "tp"),
            P("sp", None, "tp"),
            P("sp", "tp", None),
        ),
        out_specs=P("sp", "tp"),
        check_vma=False,
    )
```
